32 devices in a mesh: sp: 8 (over z, y), tp: 4 (over x, core).
Axes of the slice: x: 2, y: 2, z: 4, core: 2. Of those that a mesh axis runs over, the one named last changes fastest.
Arguments:
- residual_in: bfloat16 [8192, 2048], P(('sp', 'tp')), may hold values from -6 to 6
- queries: bfloat16 [8192, 2048], P('sp', 'tp'), may hold values from -200 to 200, as said below
- keys_values: bfloat16 [2, 8192, 1024], P(None, 'sp', 'tp'), may hold values from -6 to 6
- sink_logit: float32 [32], P('tp'), may hold values from -2 to 6
- out_weight: bfloat16 [2048, 2048], P('tp'), may hold values from -2 to 2
- norm1_gain: float32 [2048], replicated, may hold values from 0.1 to 1.9
- norm1_bias: float32 [2048], replicated, may hold values from -3 to 3
- up_weight: bfloat16 [2048, 8192], P('sp', 'tp'), may hold values from -0.125 to 0.125
- down_weight: bfloat16 [8192, 2048], P('tp', 'sp'), may hold values from -0.0625 to 0.0625
- norm2_gain: float32 [2048], replicated, may hold values from 0.1 to 1.9
- norm2_bias: float32 [2048], replicated, may hold values from -3 to 3
Outputs:
- stream_out: bfloat16 [8192, 2048], P(('sp', 'tp'))
The draws below stay inside these ranges and needn't reach their ends.
Inputs may be any that keep to these rules, and one draw needn't show every extreme that they name: `queries`: of order one mostly; some rows may be large multiples of a nearby key row.
All inputs are finite; a program needn't handle non-finite values.
Results may differ from the reference program's by a relative error of at most 0.014.
Values may be sent and summed in bfloat16 or wider, within the bound.
A program may use at most 128 MiB of HBM per device.

```python
import jax
import jax.numpy as jnp
from jax import lax

D = 2048
HEADS = 32
KV_HEADS = 16
HEAD_DIM = 64
FF = 8192
WINDOW = 128
TOK_DEV = 1024
TOKENS = 8192
N_TP = 4


def joint_draw(key):
    query = jnp.clip(jax.random.normal(jax.random.fold_in(key, 11), (TOKENS, HEADS * HEAD_DIM), jnp.float32), -5.0, 5.0)
    pairs = jnp.clip(jax.random.normal(jax.random.fold_in(key, 12), (2, TOKENS, KV_HEADS * HEAD_DIM), jnp.float32), -5.0, 5.0)
    return (query, pairs)


def draw_queries(key, part):
    return joint_draw(key)[0].astype(jnp.bfloat16)


def draw_keys_values(key, part):
    return joint_draw(key)[1].astype(jnp.bfloat16)


def levels(key, extent, split, low, top_value):
    level = 1.0
    for dim, shards_of in split:
        heights = jax.random.uniform(jax.random.fold_in(jax.random.fold_in(key, 6), dim), (shards_of,), jnp.float32, low / len(split), top_value / len(split))
        level = level * jnp.repeat(jnp.exp(heights), extent[dim] // shards_of).reshape((-1,) + (1,) * (len(extent) - 1 - dim))
    return level


def noise(rng, extent, width, most, split=(), kind=jnp.bfloat16):
    factor_of = levels(rng, extent, split, -0.22, 0.18) if split else 1.0
    values = jax.random.normal(rng, extent, jnp.float32) * width * factor_of
    return jnp.minimum(jnp.maximum(values, -most), most).astype(kind)


def setup_inputs(seed: int = 0) -> dict:
    splits = jax.random.split(jax.random.key(seed), 12)
    residual_in = noise(splits[0], (TOKENS, D), 1.0, 6.0, ((0, 32),))
    queries = draw_queries(jax.random.fold_in(splits[11], 71), 0)
    keys_values = draw_keys_values(jax.random.fold_in(splits[11], 71), 0)
    sink_logit = jnp.clip(-2.0 + 8.0 * jax.random.uniform(splits[3], (HEADS,), jnp.float32) ** levels(splits[3], (HEADS,), ((0, 4),), -0.2, 0.2), -2.0, 6.0)
    out_weight = noise(splits[4], (HEADS * HEAD_DIM, D), (6 * (HEADS * HEAD_DIM) ** -0.5), 2.0, ((0, 4),))
    norm1_gain = jnp.clip(1.0 + 0.18 * jax.random.normal(splits[5], (D,), jnp.float32), 0.1, 1.9)
    norm1_bias = noise(splits[6], (D,), 0.3, 3.0, (), jnp.float32)
    up_weight = noise(splits[7], (D, FF), D ** -0.5, 0.125, ((0, 8), (1, 4)))
    down_weight = noise(splits[8], (FF, D), FF ** -0.5, 0.0625, ((0, 4), (1, 8)))
    norm2_gain = jnp.clip(1.0 + 0.18 * jax.random.normal(splits[9], (D,), jnp.float32), 0.1, 1.9)
    norm2_bias = noise(splits[10], (D,), 0.3, 3.0, (), jnp.float32)
    return dict(residual_in=residual_in, queries=queries, keys_values=keys_values, sink_logit=sink_logit, out_weight=out_weight, norm1_gain=norm1_gain, norm1_bias=norm1_bias, up_weight=up_weight, down_weight=down_weight, norm2_gain=norm2_gain, norm2_bias=norm2_bias)


def norm_rows(values, gain, bias):
    mean = lax.optimization_barrier(jnp.mean(values, axis=-1, keepdims=True))
    centred = values - mean
    variance = lax.optimization_barrier(jnp.mean(centred * centred, axis=-1, keepdims=True))
    return (centred * lax.rsqrt(variance + 1e-06) * gain + bias).astype(jnp.bfloat16)

def reference(residual_in, queries, keys_values, sink_logit, out_weight, norm1_gain, norm1_bias, up_weight, down_weight, norm2_gain, norm2_bias):
    block = min(512, TOK_DEV)
    span = block + 2 * WINDOW
    group = HEADS // KV_HEADS
    padded = jnp.pad(keys_values, ((0, 0), (WINDOW, WINDOW), (0, 0)))
    sink = sink_logit.reshape(KV_HEADS, group, 1, 1)

    def one_block(index):
        start = (index * block).astype(jnp.int32)
        query = lax.dynamic_slice_in_dim(queries, start, block, 0).astype(jnp.float32).reshape(block, KV_HEADS, group, HEAD_DIM)
        keys = lax.dynamic_slice_in_dim(padded[0], start, span, 0).astype(jnp.float32).reshape(span, KV_HEADS, HEAD_DIM)
        values = lax.dynamic_slice_in_dim(padded[1], start, span, 0).astype(jnp.float32).reshape(span, KV_HEADS, HEAD_DIM)
        scores = jnp.einsum('qhgd,khd->hgqk', query, keys) * HEAD_DIM ** (-0.5)
        query_pos = start + jnp.arange(block, dtype=jnp.int32)
        key_pos = start - WINDOW + jnp.arange(span, dtype=jnp.int32)
        valid = (jnp.abs(key_pos[None, :] - query_pos[:, None]) <= WINDOW) & (key_pos[None, :] >= 0) & (key_pos[None, :] < TOKENS)
        scores = jnp.where(valid, scores, -jnp.inf)
        top = jnp.maximum(lax.optimization_barrier(jnp.max(scores, axis=-1, keepdims=True)), sink)
        expd = jnp.exp(scores - top)
        total = lax.optimization_barrier(jnp.sum(expd, axis=-1, keepdims=True)) + jnp.exp(sink - top)
        weights = lax.optimization_barrier((expd / total).astype(jnp.bfloat16)).astype(jnp.float32)
        mixed = jnp.einsum('hgqk,khd->qhgd', weights, values)
        return mixed.reshape(block, HEADS * HEAD_DIM).astype(jnp.bfloat16)
    attended = lax.map(one_block, jnp.arange(TOKENS // block, dtype=jnp.int32)).reshape(TOKENS, HEADS * HEAD_DIM)
    head_cols = HEADS * HEAD_DIM // N_TP
    projected = jnp.zeros((TOKENS, D), jnp.float32)
    for part in range(N_TP):
        term = jnp.dot(attended[:, part * head_cols:(part + 1) * head_cols], out_weight[part * head_cols:(part + 1) * head_cols], preferred_element_type=jnp.float32)
        projected = projected + term.astype(jnp.bfloat16).astype(jnp.float32)
    first = norm_rows(residual_in.astype(jnp.float32) + projected, norm1_gain, norm1_bias)
    hidden = jnp.dot(first, up_weight, preferred_element_type=jnp.float32)
    activation = jnp.square(jnp.maximum(hidden, 0.0)).astype(jnp.bfloat16)
    unit_cols = FF // N_TP
    branch = jnp.zeros((TOKENS, D), jnp.float32)
    for part in range(N_TP):
        term = jnp.dot(activation[:, part * unit_cols:(part + 1) * unit_cols], down_weight[part * unit_cols:(part + 1) * unit_cols], preferred_element_type=jnp.float32)
        branch = branch + term.astype(jnp.bfloat16).astype(jnp.float32)
    return norm_rows(first.astype(jnp.float32) + branch, norm2_gain, norm2_bias)
```

```python
import functools

import jax
import jax.numpy as jnp
from jax import lax
from jax.experimental import pallas as pl
from jax.experimental.pallas import tpu as pltpu
from jax.sharding import PartitionSpec as P

HEAD_DIM = 64
WINDOW = 128
BLOCK = 256


def ring_order(devices):
    return list(range(0, devices, 2)) + list(range(1, devices, 2))[::-1]


def halo(shard, axis, width):
    devices, length = lax.axis_size(axis), shard.shape[1]
    up = [(i, (i + 1) % devices) for i in range(devices - 1)]
    down = [(j, i) for i, j in up]
    before = lax.ppermute(shard[:, length - width :], axis, up)
    after = lax.ppermute(shard[:, :width], axis, down)
    return jnp.concatenate([before, shard, after], axis=1)


def norm_rows(values, gain, bias):
    mean = jnp.mean(values, axis=-1, keepdims=True)
    centred = values - mean
    variance = jnp.mean(centred * centred, axis=-1, keepdims=True)
    return (centred * lax.rsqrt(variance + 1e-06) * gain + bias).astype(jnp.bfloat16)


def attend_kernel(total, heads, group, info_ref, sink_ref, q_ref, kv_ref, w_ref, o_ref, mix_ref):
    start = pl.program_id(0) * BLOCK
    span = BLOCK + 2 * WINDOW
    rows = lax.broadcasted_iota(jnp.int32, (BLOCK, span), 0)
    cols = lax.broadcasted_iota(jnp.int32, (BLOCK, span), 1)
    pos = cols + (info_ref[0] + start - WINDOW)
    valid = (cols >= rows) & (cols - rows <= 2 * WINDOW) & (pos >= 0) & (pos < total)
    begin = pl.multiple_of(start, BLOCK)
    for kv in range(heads // group):
        lanes = slice(kv * HEAD_DIM, (kv + 1) * HEAD_DIM)
        keys = kv_ref[0, pl.ds(begin, span), lanes]
        values = kv_ref[1, pl.ds(begin, span), lanes]
        for sub in range(group):
            head = kv * group + sub
            mine = slice(head * HEAD_DIM, (head + 1) * HEAD_DIM)
            query = q_ref[:, mine]
            scores = lax.dot_general(
                query, keys, (((1,), (1,)), ((), ())), preferred_element_type=jnp.float32
            ) * HEAD_DIM ** (-0.5)
            scores = jnp.where(valid, scores, -jnp.inf)
            sink = sink_ref[head]
            top = jnp.maximum(jnp.max(scores, axis=-1, keepdims=True), sink)
            expd = jnp.exp(scores - top)
            denom = jnp.sum(expd, axis=-1, keepdims=True) + jnp.exp(sink - top)
            weights = (expd * (1.0 / denom)).astype(jnp.bfloat16)
            mixed = jnp.dot(weights, values, preferred_element_type=jnp.float32)
            mix_ref[:, mine] = mixed.astype(jnp.bfloat16)
    o_ref[...] = jnp.dot(
        mix_ref[...], w_ref[...], preferred_element_type=jnp.float32
    ).astype(jnp.bfloat16)


def attend(queries, padded, sink_logit, out_weight, offset, total):
    rows, width = queries.shape
    heads = width // HEAD_DIM
    group = heads // (padded.shape[2] // HEAD_DIM)
    depth = out_weight.shape[1]
    span = BLOCK + 2 * WINDOW
    flops = 2 * rows * width * depth + 4 * rows * span * width
    return pl.pallas_call(
        functools.partial(attend_kernel, total, heads, group),
        grid=(rows // BLOCK,),
        in_specs=[
            pl.BlockSpec(memory_space=pltpu.SMEM),
            pl.BlockSpec(memory_space=pltpu.SMEM),
            pl.BlockSpec((BLOCK, width), lambda i: (i, 0)),
            pl.BlockSpec(padded.shape, lambda i: (0, 0, 0)),
            pl.BlockSpec(out_weight.shape, lambda i: (0, 0)),
        ],
        out_specs=pl.BlockSpec((BLOCK, depth), lambda i: (i, 0)),
        out_shape=jax.ShapeDtypeStruct((rows, depth), jnp.bfloat16),
        scratch_shapes=[pltpu.VMEM((BLOCK, width), jnp.bfloat16)],
        compiler_params=pltpu.CompilerParams(vmem_limit_bytes=40 * 2**20),
        cost_estimate=pl.CostEstimate(
            flops=flops * 3, bytes_accessed=12 * 2**20, transcendentals=rows * span * heads
        ),
        name="attend",
    )(offset.reshape(1), sink_logit, queries, padded, out_weight)


def up_kernel(owners, info_ref, rows_ref, *refs):
    *blocks, out_ref = refs
    tile = 256
    for at in range(0, rows_ref.shape[0], tile):
        total = None
        for k, block in enumerate(blocks):
            depth = block.shape[0]
            begin = pl.multiple_of(info_ref[k], depth)
            term = jnp.dot(
                rows_ref[at : at + tile, pl.ds(begin, depth)],
                block[...],
                preferred_element_type=jnp.float32,
            )
            total = term if total is None else total + term
        out_ref[at : at + tile, :] = jnp.square(jnp.maximum(total, 0.0)).astype(jnp.bfloat16)


def up_project(rows, blocks, starts):
    count, depth = rows.shape
    hidden = blocks[0].shape[1]
    tile = min(512, hidden)
    return pl.pallas_call(
        functools.partial(up_kernel, len(blocks)),
        grid=(hidden // tile,),
        in_specs=[
            pl.BlockSpec(memory_space=pltpu.SMEM),
            pl.BlockSpec(rows.shape, lambda j: (0, 0)),
        ]
        + [pl.BlockSpec((b.shape[0], tile), lambda j: (0, j)) for b in blocks],
        out_specs=pl.BlockSpec((count, tile), lambda j: (0, j)),
        out_shape=jax.ShapeDtypeStruct((count, hidden), jnp.bfloat16),
        compiler_params=pltpu.CompilerParams(vmem_limit_bytes=40 * 2**20),
        cost_estimate=pl.CostEstimate(
            flops=2 * count * depth * hidden, bytes_accessed=16 * 2**20, transcendentals=0
        ),
        name="up_project",
    )(starts, rows, *blocks)


def down_kernel(rows_ref, *refs):
    *blocks, out_ref = refs
    at = 0
    for block in blocks:
        wide = block.shape[1]
        out_ref[:, at : at + wide] = jnp.dot(
            rows_ref[...], block[...], preferred_element_type=jnp.float32
        ).astype(jnp.bfloat16)
        at += wide


def down_project(rows, blocks):
    count, hidden = rows.shape
    depth = sum(b.shape[1] for b in blocks)
    tile = min(256, count)
    return pl.pallas_call(
        down_kernel,
        grid=(count // tile,),
        in_specs=[pl.BlockSpec((tile, hidden), lambda i: (i, 0))]
        + [pl.BlockSpec(b.shape, lambda i: (0, 0)) for b in blocks],
        out_specs=pl.BlockSpec((tile, depth), lambda i: (i, 0)),
        out_shape=jax.ShapeDtypeStruct((count, depth), jnp.bfloat16),
        compiler_params=pltpu.CompilerParams(vmem_limit_bytes=40 * 2**20),
        cost_estimate=pl.CostEstimate(
            flops=2 * count * depth * hidden, bytes_accessed=16 * 2**20, transcendentals=0
        ),
        name="down_project",
    )(rows, *blocks)


def last_norm_kernel(count, info_ref, first_ref, gain_ref, bias_ref, branch_ref, out_ref, sum_ref):
    wide = branch_ref.shape[1] // count
    for k in range(count):
        cols = pl.ds(pl.multiple_of(info_ref[k], wide), wide)
        sum_ref[:, cols] = first_ref[:, cols].astype(jnp.float32) + branch_ref[
            :, k * wide : (k + 1) * wide
        ].astype(jnp.float32)
    out_ref[...] = norm_rows(sum_ref[...], gain_ref[...], bias_ref[...])


def last_norm(first, branch, gain, bias, starts):
    rows, depth = first.shape
    tile = min(128, rows)
    return pl.pallas_call(
        functools.partial(last_norm_kernel, starts.shape[0]),
        grid=(rows // tile,),
        in_specs=[
            pl.BlockSpec(memory_space=pltpu.SMEM),
            pl.BlockSpec((tile, depth), lambda i: (i, 0)),
            pl.BlockSpec((1, depth), lambda i: (0, 0)),
            pl.BlockSpec((1, depth), lambda i: (0, 0)),
            pl.BlockSpec((tile, depth), lambda i: (i, 0)),
        ],
        out_specs=pl.BlockSpec((tile, depth), lambda i: (i, 0)),
        out_shape=jax.ShapeDtypeStruct((rows, depth), jnp.bfloat16),
        scratch_shapes=[pltpu.VMEM((tile, depth), jnp.float32)],
        cost_estimate=pl.CostEstimate(
            flops=rows * depth * 10, bytes_accessed=4 * 2**20, transcendentals=0
        ),
        name="last_norm",
    )(starts, first, gain.reshape(1, -1), bias.reshape(1, -1), branch)


def on_device(
    residual_in,
    queries,
    keys_values,
    sink_logit,
    out_weight,
    norm1_gain,
    norm1_bias,
    up_weight,
    down_weight,
    norm2_gain,
    norm2_bias,
):
    devices = lax.axis_size("sp")
    order = ring_order(devices)
    right = [(order[i], order[(i + 1) % devices]) for i in range(devices)]
    left = [(j, i) for i, j in right]
    far = devices // 2

    def hop(h, back, ahead):
        if h > far:
            return None, None
        if 2 * h == devices:
            half = back.shape[0] // 2
            return (
                lax.ppermute(back[:half], "sp", right),
                lax.ppermute(ahead[half:], "sp", left),
            )
        return lax.ppermute(back, "sp", right), lax.ppermute(ahead, "sp", left)

    tok_rows = queries.shape[0]
    me = lax.axis_index("sp")
    offset = me * tok_rows
    total = tok_rows * devices

    place = [0] * devices
    for p, d in enumerate(order):
        place[d] = p
    steps = [0]
    for h in range(1, far + 1):
        steps.append(-h)
        if 2 * h != devices:
            steps.append(h)
    table = jnp.array(
        [[order[(place[d] + s) % devices] for s in steps] for d in range(devices)], jnp.int32
    )
    owners = lax.dynamic_index_in_dim(table, me, 0, keepdims=False)
    starts = owners * up_weight.shape[0]

    if up_weight.shape[0] % 128:
        up_weight = lax.all_gather(up_weight, "sp", axis=0, tiled=True)
        down_weight = lax.all_gather(down_weight, "sp", axis=1, tiled=True)
        far, starts = 0, jnp.zeros((1,), jnp.int32)

    ups, downs = [up_weight], [down_weight]
    state = {"up": (up_weight, up_weight), "down": (down_weight, down_weight)}

    def advance(name, h):
        state[name] = hop(h, *state[name])

    def settle(name, h, *others):
        got = state[name]
        if got[0] is None:
            return others
        out = lax.optimization_barrier((*got, *others))
        state[name] = out[:2]
        blocks = ups if name == "up" else downs
        if 2 * h == devices:
            blocks.append(jnp.concatenate(out[:2], axis=0))
        else:
            blocks.extend(out[:2])
        return out[2:]

    advance("up", 1)
    advance("down", 1)
    padded = halo(keys_values, "sp", WINDOW)
    partial = attend(queries, padded, sink_logit, out_weight, offset, total)
    (partial,) = settle("up", 1, partial)
    advance("up", 2)
    (partial,) = settle("down", 1, partial)
    advance("down", 2)
    projected = lax.psum_scatter(partial, "tp", scatter_dimension=0, tiled=True)
    first = norm_rows(
        residual_in.astype(jnp.float32) + projected.astype(jnp.float32), norm1_gain, norm1_bias
    )
    (first,) = settle("up", 2, first)
    advance("up", 3)
    (first,) = settle("down", 2, first)
    advance("down", 3)
    rows = lax.all_gather(first, "tp", axis=0, tiled=True)
    (rows,) = settle("up", 3, rows)
    advance("up", 4)
    (rows,) = settle("up", 4, rows)
    for h in range(5, far + 1):
        advance("up", h)
        (rows,) = settle("up", h, rows)
    activation = up_project(rows, ups, starts)
    (activation,) = settle("down", 3, activation)
    early = len(downs)
    advance("down", 4)
    piece = down_project(activation, downs[:early])
    pieces = [lax.psum_scatter(piece, "tp", scatter_dimension=0, tiled=True)]
    (activation,) = settle("down", 4, activation)
    for h in range(5, far + 1):
        advance("down", h)
        (activation,) = settle("down", h, activation)
    if len(downs) > early:
        piece = down_project(activation, downs[early:])
        pieces.append(lax.psum_scatter(piece, "tp", scatter_dimension=0, tiled=True))
    branch = jnp.concatenate(pieces, axis=1)
    return last_norm(first, branch, norm2_gain, norm2_bias, starts)


def solution(mesh):
    return jax.shard_map(
        on_device,
        mesh=mesh,
        in_specs=(
            P(("sp", "tp"), None),
            P("sp", "tp"),
            P(None, "sp", "tp"),
            P("tp"),
            P("tp", None),
            P(),
            P(),
            P("sp", "tp"),
            P("tp", "sp"),
            P(),
            P(),
        ),
        out_specs=P(("sp", "tp"), None),
        check_vma=False,
    )
```

```python
import functools

import jax
import jax.numpy as jnp
from jax import lax
from jax.experimental import pallas as pl
from jax.experimental.pallas import tpu as pltpu
from jax.sharding import PartitionSpec as P

HEAD_DIM = 64
WINDOW = 128
BLOCK = 256


def ring_order(devices):
    return list(range(0, devices, 2)) + list(range(1, devices, 2))[::-1]


def halo(shard, axis, width):
    devices, length = lax.axis_size(axis), shard.shape[1]
    up = [(i, (i + 1) % devices) for i in range(devices - 1)]
    down = [(j, i) for i, j in up]
    before = lax.ppermute(shard[:, length - width :], axis, up)
    after = lax.ppermute(shard[:, :width], axis, down)
    return jnp.concatenate([before, shard, after], axis=1)


def norm_rows(values, gain, bias):
    mean = jnp.mean(values, axis=-1, keepdims=True)
    centred = values - mean
    variance = jnp.mean(centred * centred, axis=-1, keepdims=True)
    return (centred * lax.rsqrt(variance + 1e-06) * gain + bias).astype(jnp.bfloat16)


def attend_kernel(total, heads, group, info_ref, sink_ref, q_ref, kv_ref, o_ref):
    start = pl.program_id(0) * BLOCK
    span = BLOCK + 2 * WINDOW
    rows = lax.broadcasted_iota(jnp.int32, (BLOCK, span), 0)
    cols = lax.broadcasted_iota(jnp.int32, (BLOCK, span), 1)
    pos = cols + (info_ref[0] + start - WINDOW)
    valid = (cols >= rows) & (cols - rows <= 2 * WINDOW) & (pos >= 0) & (pos < total)
    begin = pl.multiple_of(start, BLOCK)
    for kv in range(heads // group):
        lanes = slice(kv * HEAD_DIM, (kv + 1) * HEAD_DIM)
        keys = kv_ref[0, pl.ds(begin, span), lanes]
        values = kv_ref[1, pl.ds(begin, span), lanes]
        for sub in range(group):
            head = kv * group + sub
            mine = slice(head * HEAD_DIM, (head + 1) * HEAD_DIM)
            query = q_ref[:, mine]
            scores = lax.dot_general(
                query, keys, (((1,), (1,)), ((), ())), preferred_element_type=jnp.float32
            ) * HEAD_DIM ** (-0.5)
            scores = jnp.where(valid, scores, -jnp.inf)
            sink = sink_ref[head]
            top = jnp.maximum(jnp.max(scores, axis=-1, keepdims=True), sink)
            expd = jnp.exp(scores - top)
            denom = jnp.sum(expd, axis=-1, keepdims=True) + jnp.exp(sink - top)
            weights = (expd * (1.0 / denom)).astype(jnp.bfloat16)
            mixed = jnp.dot(weights, values, preferred_element_type=jnp.float32)
            o_ref[:, mine] = mixed.astype(jnp.bfloat16)


def attend(queries, padded, sink_logit, offset, total):
    rows, width = queries.shape
    heads = width // HEAD_DIM
    group = heads // (padded.shape[2] // HEAD_DIM)
    span = BLOCK + 2 * WINDOW
    flops = 4 * rows * span * width
    return pl.pallas_call(
        functools.partial(attend_kernel, total, heads, group),
        grid=(rows // BLOCK,),
        in_specs=[
            pl.BlockSpec(memory_space=pltpu.SMEM),
            pl.BlockSpec(memory_space=pltpu.SMEM),
            pl.BlockSpec((BLOCK, width), lambda i: (i, 0)),
            pl.BlockSpec(padded.shape, lambda i: (0, 0, 0)),
        ],
        out_specs=pl.BlockSpec((BLOCK, width), lambda i: (i, 0)),
        out_shape=jax.ShapeDtypeStruct((rows, width), jnp.bfloat16),
        compiler_params=pltpu.CompilerParams(vmem_limit_bytes=40 * 2**20),
        cost_estimate=pl.CostEstimate(
            flops=flops * 20, bytes_accessed=12 * 2**20, transcendentals=rows * span * heads
        ),
        name="attend",
    )(offset.reshape(1), sink_logit, queries, padded)


def up_kernel(owners, info_ref, rows_ref, *refs):
    *blocks, out_ref = refs
    tile = 256
    for at in range(0, rows_ref.shape[0], tile):
        total = None
        for k, block in enumerate(blocks):
            depth = block.shape[0]
            begin = pl.multiple_of(info_ref[k], depth)
            term = jnp.dot(
                rows_ref[at : at + tile, pl.ds(begin, depth)],
                block[...],
                preferred_element_type=jnp.float32,
            )
            total = term if total is None else total + term
        out_ref[at : at + tile, :] = jnp.square(jnp.maximum(total, 0.0)).astype(jnp.bfloat16)


def up_project(rows, blocks, starts):
    count, depth = rows.shape
    hidden = blocks[0].shape[1]
    tile = min(512, hidden)
    return pl.pallas_call(
        functools.partial(up_kernel, len(blocks)),
        grid=(hidden // tile,),
        in_specs=[
            pl.BlockSpec(memory_space=pltpu.SMEM),
            pl.BlockSpec(rows.shape, lambda j: (0, 0)),
        ]
        + [pl.BlockSpec((b.shape[0], tile), lambda j: (0, j)) for b in blocks],
        out_specs=pl.BlockSpec((count, tile), lambda j: (0, j)),
        out_shape=jax.ShapeDtypeStruct((count, hidden), jnp.bfloat16),
        compiler_params=pltpu.CompilerParams(vmem_limit_bytes=40 * 2**20),
        cost_estimate=pl.CostEstimate(
            flops=2 * count * depth * hidden, bytes_accessed=16 * 2**20, transcendentals=0
        ),
        name="up_project",
    )(starts, rows, *blocks)


MESH = pl.DeviceIdType.MESH


def remote(src, dst, send, recv, target):
    return pltpu.make_async_remote_copy(
        src_ref=src,
        dst_ref=dst,
        send_sem=send,
        recv_sem=recv,
        device_id={"tp": target},
        device_id_type=MESH,
    )


def places():
    me = lax.axis_index("tp")
    side, core = me // 2, me % 2
    return me, 2 * side + (1 - core), 2 * (1 - side) + core, 2 * (1 - side) + (1 - core)


def greet(*others):
    barrier = pltpu.get_barrier_semaphore()
    for other in others:
        pl.semaphore_signal(barrier, inc=1, device_id={"tp": other}, device_id_type=MESH)
    pl.semaphore_wait(barrier, len(others))


def ring_place(index, devices):
    odd = index % 2
    return (1 - odd) * (index // 2) + odd * (devices - 1 - index // 2)


def ring_device(place, devices):
    half = (devices + 1) // 2
    back = place // half
    return (1 - back) * (2 * place) + back * (2 * (devices - 1 - place) + 1)


def scatter_kernel(
    steps, pieces, rows_ref, res_ref, gain_ref, bias_ref, *refs
):
    *blocks, out_ref, part, inc, total, got, send, recv = refs
    me, partner, across, diagonal = places()
    block_rows = out_ref.shape[0]
    size = block_rows // pieces
    devices = lax.axis_size("sp")
    spot = ring_place(lax.axis_index("sp"), devices)
    greet(partner, across)

    def compute(slot, owner, s):
        begin = pl.multiple_of(owner * block_rows + s * size, size)
        mine = rows_ref[pl.ds(begin, size), :]
        for step, block in zip(steps, blocks):
            wide = block.shape[1]
            at = 0
            if len(blocks) > 1:
                at = ring_device((spot + step + devices) % devices, devices) * wide
                at = pl.multiple_of(at, wide)
            part[slot, pl.ds(s * size, size), pl.ds(at, wide)] = jnp.dot(
                mine, block[...], preferred_element_type=jnp.float32
            ).astype(jnp.bfloat16)

    def copy(kind, s):
        cut = pl.ds(s * size, size)
        if kind == 0:
            src, dst, target = part.at[0, cut], inc.at[0, cut], partner
        elif kind == 1:
            src, dst, target = total.at[cut], got.at[cut], across
        else:
            src, dst, target = part.at[2, cut], inc.at[1, cut], partner
        return remote(src, dst, send.at[kind, s], recv.at[kind, s], target)

    for s in range(pieces):
        cut = pl.ds(s * size, size)
        compute(0, diagonal, s)
        copy(0, s).start()
        compute(1, across, s)
        copy(0, s).wait_recv()
        total[cut, :] = (
            part[1, cut, :].astype(jnp.float32) + inc[0, cut, :].astype(jnp.float32)
        ).astype(jnp.bfloat16)
        copy(1, s).start()
    for s in range(pieces):
        compute(2, partner, s)
        copy(2, s).start()
    for s in range(pieces):
        compute(3, me, s)
    for s in range(pieces):
        cut = pl.ds(s * size, size)
        copy(2, s).wait_recv()
        here = (
            res_ref[cut, :].astype(jnp.float32)
            + part[3, cut, :].astype(jnp.float32)
            + inc[1, cut, :].astype(jnp.float32)
        )
        copy(1, s).wait_recv()
        out_ref[cut, :] = norm_rows(
            here + got[cut, :].astype(jnp.float32), gain_ref[...], bias_ref[...]
        )
    for s in range(pieces):
        for kind in range(3):
            copy(kind, s).wait_send()


def scatter_norm(rows, blocks, steps, residual, gain, bias, pieces, ident):
    count, width = rows.shape
    own, depth = residual.shape
    return pl.pallas_call(
        functools.partial(scatter_kernel, steps, pieces),
        in_specs=[pl.BlockSpec(memory_space=pltpu.VMEM)] * (4 + len(blocks)),
        out_specs=pl.BlockSpec(memory_space=pltpu.VMEM),
        out_shape=jax.ShapeDtypeStruct((own, depth), jnp.bfloat16),
        scratch_shapes=[
            pltpu.VMEM((4, own, depth), jnp.bfloat16),
            pltpu.VMEM((2, own, depth), jnp.bfloat16),
            pltpu.VMEM((own, depth), jnp.bfloat16),
            pltpu.VMEM((own, depth), jnp.bfloat16),
            pltpu.SemaphoreType.DMA((3, pieces)),
            pltpu.SemaphoreType.DMA((3, pieces)),
        ],
        compiler_params=pltpu.CompilerParams(
            collective_id=ident, has_side_effects=True, vmem_limit_bytes=48 * 2**20
        ),
        cost_estimate=pl.CostEstimate(
            flops=25 * 10**9, bytes_accessed=16 * 2**20, transcendentals=0
        ),
        name=f"scatter_norm_{ident}",
    )(rows, residual, gain.reshape(1, -1), bias.reshape(1, -1), *blocks)


def gather_kernel(pieces, first_ref, out_ref, local, send, recv):
    me, partner, across, _ = places()
    block_rows = first_ref.shape[0]
    size = block_rows // pieces
    greet(partner, across)

    def copy(kind, s):
        owner = across if kind == 2 else me
        cut = pl.ds(pl.multiple_of(owner * block_rows + s * size, size), size)
        src = out_ref.at[cut] if kind == 2 else first_ref.at[pl.ds(s * size, size)]
        target = across if kind == 0 else partner
        return remote(src, out_ref.at[cut], send.at[kind, s], recv.at[kind, s], target)

    for s in range(pieces):
        copy(0, s).start()
    for s in range(pieces):
        copy(1, s).start()
    keep = pltpu.make_async_copy(
        first_ref,
        out_ref.at[pl.ds(pl.multiple_of(me * block_rows, block_rows), block_rows)],
        local,
    )
    keep.start()
    for s in range(pieces):
        copy(0, s).wait_recv()
        copy(2, s).start()
    for s in range(pieces):
        copy(1, s).wait_recv()
        copy(2, s).wait_recv()
    for s in range(pieces):
        for kind in range(3):
            copy(kind, s).wait_send()
    keep.wait()


def gather_rows(first, groups, pieces, ident):
    own, depth = first.shape
    return pl.pallas_call(
        functools.partial(gather_kernel, pieces),
        in_specs=[pl.BlockSpec(memory_space=pltpu.VMEM)],
        out_specs=pl.BlockSpec(memory_space=pltpu.VMEM),
        out_shape=jax.ShapeDtypeStruct((own * groups, depth), jnp.bfloat16),
        scratch_shapes=[
            pltpu.SemaphoreType.DMA,
            pltpu.SemaphoreType.DMA((3, pieces)),
            pltpu.SemaphoreType.DMA((3, pieces)),
        ],
        compiler_params=pltpu.CompilerParams(
            collective_id=ident, has_side_effects=True, vmem_limit_bytes=24 * 2**20
        ),
        cost_estimate=pl.CostEstimate(
            flops=25 * 10**9, bytes_accessed=5 * 2**20, transcendentals=0
        ),
        name="gather_rows",
    )(first)


def on_device(
    residual_in,
    queries,
    keys_values,
    sink_logit,
    out_weight,
    norm1_gain,
    norm1_bias,
    up_weight,
    down_weight,
    norm2_gain,
    norm2_bias,
):
    devices = lax.axis_size("sp")
    order = ring_order(devices)
    right = [(order[i], order[(i + 1) % devices]) for i in range(devices)]
    left = [(j, i) for i, j in right]
    far = devices // 2

    def hop(h, back, ahead):
        if h > far:
            return None, None
        if 2 * h == devices:
            half = back.shape[0] // 2
            return (
                lax.ppermute(back[:half], "sp", right),
                lax.ppermute(ahead[half:], "sp", left),
            )
        return lax.ppermute(back, "sp", right), lax.ppermute(ahead, "sp", left)

    tok_rows = queries.shape[0]
    me = lax.axis_index("sp")
    offset = me * tok_rows
    total = tok_rows * devices

    place = [0] * devices
    for p, d in enumerate(order):
        place[d] = p
    steps = [0]
    for h in range(1, far + 1):
        steps.append(-h)
        if 2 * h != devices:
            steps.append(h)
    table = jnp.array(
        [[order[(place[d] + s) % devices] for s in steps] for d in range(devices)], jnp.int32
    )
    owners = lax.dynamic_index_in_dim(table, me, 0, keepdims=False)
    starts = owners * up_weight.shape[0]

    if up_weight.shape[0] % 128:
        up_weight = lax.all_gather(up_weight, "sp", axis=0, tiled=True)
        down_weight = lax.all_gather(down_weight, "sp", axis=1, tiled=True)
        far, starts = 0, jnp.zeros((1,), jnp.int32)

    ups, downs = [up_weight], [down_weight]
    state = {"up": (up_weight, up_weight), "down": (down_weight, down_weight)}

    def advance(name, h):
        state[name] = hop(h, *state[name])

    def settle(name, h, *others):
        got = state[name]
        if got[0] is None or h > far:
            return others
        out = lax.optimization_barrier((*got, *others))
        state[name] = out[:2]
        blocks = ups if name == "up" else downs
        if 2 * h == devices:
            blocks.append(jnp.concatenate(out[:2], axis=0))
        else:
            blocks.extend(out[:2])
        return out[2:]

    advance("up", 1)
    advance("down", 1)
    padded = halo(keys_values, "sp", WINDOW)
    attended = attend(queries, padded, sink_logit, offset, total)
    (attended,) = settle("up", 1, attended)
    advance("up", 2)
    first = scatter_norm(
        attended, [out_weight], [0], residual_in, norm1_gain, norm1_bias, 2, 0
    )
    (first,) = settle("down", 1, first)
    advance("down", 2)
    rows = gather_rows(first, lax.axis_size("tp"), 4, 1)
    (rows,) = settle("up", 2, rows)
    advance("up", 3)
    (rows,) = settle("down", 2, rows)
    (rows, *ready) = settle("up", 3, rows, *state["down"])
    state["down"] = tuple(ready)
    for h in range(4, far + 1):
        advance("up", h)
        if h == 4:
            advance("down", 3)
        (rows,) = settle("up", h, rows)
    activation = up_project(rows, ups, starts)
    (activation,) = settle("down", 3, activation)
    for h in range(4, far + 1):
        advance("down", h)
        (activation,) = settle("down", h, activation)
    return scatter_norm(
        activation, downs, steps, first, norm2_gain, norm2_bias, 2, 2
    )


def solution(mesh):
    return jax.shard_map(
        on_device,
        mesh=mesh,
        in_specs=(
            P(("sp", "tp"), None),
            P("sp", "tp"),
            P(None, "sp", "tp"),
            P("tp"),
            P("tp", None),
            P(),
            P(),
            P("sp", "tp"),
            P("tp", "sp"),
            P(),
            P(),
        ),
        out_specs=P(("sp", "tp"), None),
        check_vma=False,
    )
```

```python
import functools

import jax
import jax.numpy as jnp
from jax import lax
from jax.experimental import pallas as pl
from jax.experimental.pallas import tpu as pltpu
from jax.sharding import PartitionSpec as P

HEAD_DIM = 64
WINDOW = 128
BLOCK = 256


def ring_order(devices):
    return list(range(0, devices, 2)) + list(range(1, devices, 2))[::-1]


def halo(shard, axis, width):
    devices, length = lax.axis_size(axis), shard.shape[1]
    up = [(i, (i + 1) % devices) for i in range(devices - 1)]
    down = [(j, i) for i, j in up]
    before = lax.ppermute(shard[:, length - width :], axis, up)
    after = lax.ppermute(shard[:, :width], axis, down)
    return jnp.concatenate([before, shard, after], axis=1)


def norm_rows(values, gain, bias):
    mean = jnp.mean(values, axis=-1, keepdims=True)
    centred = values - mean
    variance = jnp.mean(centred * centred, axis=-1, keepdims=True)
    return (centred * lax.rsqrt(variance + 1e-06) * gain + bias).astype(jnp.bfloat16)


def attend_kernel(total, heads, group, info_ref, sink_ref, q_ref, kv_ref, o_ref):
    start = pl.program_id(0) * BLOCK
    span = BLOCK + 2 * WINDOW
    rows = lax.broadcasted_iota(jnp.int32, (BLOCK, span), 0)
    cols = lax.broadcasted_iota(jnp.int32, (BLOCK, span), 1)
    pos = cols + (info_ref[0] + start - WINDOW)
    valid = (cols >= rows) & (cols - rows <= 2 * WINDOW) & (pos >= 0) & (pos < total)
    begin = pl.multiple_of(start, BLOCK)
    for kv in range(heads // group):
        lanes = slice(kv * HEAD_DIM, (kv + 1) * HEAD_DIM)
        keys = kv_ref[0, pl.ds(begin, span), lanes]
        values = kv_ref[1, pl.ds(begin, span), lanes]
        for sub in range(group):
            head = kv * group + sub
            mine = slice(head * HEAD_DIM, (head + 1) * HEAD_DIM)
            query = q_ref[:, mine]
            scores = lax.dot_general(
                query, keys, (((1,), (1,)), ((), ())), preferred_element_type=jnp.float32
            ) * HEAD_DIM ** (-0.5)
            scores = jnp.where(valid, scores, -jnp.inf)
            sink = sink_ref[head]
            top = jnp.maximum(jnp.max(scores, axis=-1, keepdims=True), sink)
            expd = jnp.exp(scores - top)
            denom = jnp.sum(expd, axis=-1, keepdims=True) + jnp.exp(sink - top)
            weights = (expd * (1.0 / denom)).astype(jnp.bfloat16)
            mixed = jnp.dot(weights, values, preferred_element_type=jnp.float32)
            o_ref[:, mine] = mixed.astype(jnp.bfloat16)


def attend(queries, padded, sink_logit, offset, total):
    rows, width = queries.shape
    heads = width // HEAD_DIM
    group = heads // (padded.shape[2] // HEAD_DIM)
    span = BLOCK + 2 * WINDOW
    flops = 4 * rows * span * width
    return pl.pallas_call(
        functools.partial(attend_kernel, total, heads, group),
        grid=(rows // BLOCK,),
        in_specs=[
            pl.BlockSpec(memory_space=pltpu.SMEM),
            pl.BlockSpec(memory_space=pltpu.SMEM),
            pl.BlockSpec((BLOCK, width), lambda i: (i, 0)),
            pl.BlockSpec(padded.shape, lambda i: (0, 0, 0)),
        ],
        out_specs=pl.BlockSpec((BLOCK, width), lambda i: (i, 0)),
        out_shape=jax.ShapeDtypeStruct((rows, width), jnp.bfloat16),
        compiler_params=pltpu.CompilerParams(vmem_limit_bytes=40 * 2**20),
        cost_estimate=pl.CostEstimate(
            flops=flops * 20, bytes_accessed=12 * 2**20, transcendentals=rows * span * heads
        ),
        name="attend",
    )(offset.reshape(1), sink_logit, queries, padded)


def up_kernel(owners, info_ref, rows_ref, *refs):
    *blocks, out_ref = refs
    tile = 256
    for at in range(0, rows_ref.shape[0], tile):
        total = None
        for k, block in enumerate(blocks):
            depth = block.shape[0]
            begin = pl.multiple_of(info_ref[k], depth)
            term = jnp.dot(
                rows_ref[at : at + tile, pl.ds(begin, depth)],
                block[...],
                preferred_element_type=jnp.float32,
            )
            total = term if total is None else total + term
        out_ref[at : at + tile, :] = jnp.square(jnp.maximum(total, 0.0)).astype(jnp.bfloat16)


def up_project(rows, blocks, starts):
    count, depth = rows.shape
    hidden = blocks[0].shape[1]
    tile = min(512, hidden)
    return pl.pallas_call(
        functools.partial(up_kernel, len(blocks)),
        grid=(hidden // tile,),
        in_specs=[
            pl.BlockSpec(memory_space=pltpu.SMEM),
            pl.BlockSpec(rows.shape, lambda j: (0, 0)),
        ]
        + [pl.BlockSpec((b.shape[0], tile), lambda j: (0, j)) for b in blocks],
        out_specs=pl.BlockSpec((count, tile), lambda j: (0, j)),
        out_shape=jax.ShapeDtypeStruct((count, hidden), jnp.bfloat16),
        compiler_params=pltpu.CompilerParams(vmem_limit_bytes=40 * 2**20),
        cost_estimate=pl.CostEstimate(
            flops=2 * count * depth * hidden, bytes_accessed=16 * 2**20, transcendentals=0
        ),
        name="up_project",
    )(starts, rows, *blocks)


MESH = pl.DeviceIdType.MESH


def remote(src, dst, send, recv, target):
    return pltpu.make_async_remote_copy(
        src_ref=src,
        dst_ref=dst,
        send_sem=send,
        recv_sem=recv,
        device_id={"tp": target},
        device_id_type=MESH,
    )


def places():
    me = lax.axis_index("tp")
    side, core = me // 2, me % 2
    return me, 2 * side + (1 - core), 2 * (1 - side) + core, 2 * (1 - side) + (1 - core)


def greet(*others):
    barrier = pltpu.get_barrier_semaphore()
    for other in others:
        pl.semaphore_signal(barrier, inc=1, device_id={"tp": other}, device_id_type=MESH)
    pl.semaphore_wait(barrier, len(others))


def ring_place(index, devices):
    odd = index % 2
    return (1 - odd) * (index // 2) + odd * (devices - 1 - index // 2)


def ring_device(place, devices):
    half = (devices + 1) // 2
    back = place // half
    return (1 - back) * (2 * place) + back * (2 * (devices - 1 - place) + 1)


def scatter_kernel(steps, before, final, pieces, rows_ref, *refs):
    refs = list(refs)
    if final:
        res_ref, gain_ref, bias_ref = refs[:3]
        refs = refs[3:]
    if before:
        before_ref = refs.pop(0)
    *blocks, out_ref, part, inc, total, got, whole, send, recv = refs
    me, partner, across, diagonal = places()
    block_rows = out_ref.shape[0]
    size = block_rows // pieces
    wide = blocks[0].shape[1]
    devices = lax.axis_size("sp")
    spot = ring_place(lax.axis_index("sp"), devices)
    greet(partner, across)

    def compute(slot, owner, s):
        begin = pl.multiple_of(owner * block_rows + s * size, size)
        mine = rows_ref[pl.ds(begin, size), :]
        for k, block in enumerate(blocks):
            part[slot, pl.ds(s * size, size), k * wide : (k + 1) * wide] = jnp.dot(
                mine, block[...], preferred_element_type=jnp.float32
            ).astype(jnp.bfloat16)

    def copy(kind, s):
        cut = pl.ds(s * size, size)
        if kind == 0:
            src, dst, target = part.at[0, cut], inc.at[0, cut], partner
        elif kind == 1:
            src, dst, target = total.at[cut], got.at[cut], across
        else:
            src, dst, target = part.at[2, cut], inc.at[1, cut], partner
        return remote(src, dst, send.at[kind, s], recv.at[kind, s], target)

    def column(step):
        if wide == whole.shape[1]:
            return pl.ds(0, wide)
        at = ring_device((spot + step + devices) % devices, devices) * wide
        return pl.ds(pl.multiple_of(at, wide), wide)

    for s in range(pieces):
        cut = pl.ds(s * size, size)
        compute(0, diagonal, s)
        copy(0, s).start()
        compute(1, across, s)
        copy(0, s).wait_recv()
        total[cut, :] = (
            part[1, cut, :].astype(jnp.float32) + inc[0, cut, :].astype(jnp.float32)
        ).astype(jnp.bfloat16)
        copy(1, s).start()
    for s in range(pieces):
        compute(2, partner, s)
        copy(2, s).start()
    for s in range(pieces):
        compute(3, me, s)
    for s in range(pieces):
        copy(2, s).wait_recv()
        if final:
            for k, step in enumerate(before):
                at = column(step)
                cut = pl.ds(s * size, size)
                whole[cut, at] = (
                    res_ref[cut, at].astype(jnp.float32)
                    + before_ref[cut, k * wide : (k + 1) * wide]
                )
    for s in range(pieces):
        cut = pl.ds(s * size, size)
        copy(1, s).wait_recv()
        for k, step in enumerate(steps):
            mine = slice(k * wide, (k + 1) * wide)
            here = (
                part[3, cut, mine].astype(jnp.float32)
                + inc[1, cut, mine].astype(jnp.float32)
                + got[cut, mine].astype(jnp.float32)
            )
            if final:
                at = column(step)
                whole[cut, at] = res_ref[cut, at].astype(jnp.float32) + here
            else:
                out_ref[cut, mine] = here
        if final:
            out_ref[cut, :] = norm_rows(whole[cut, :], gain_ref[...], bias_ref[...])
    for s in range(pieces):
        for kind in range(3):
            copy(kind, s).wait_send()


def scatter(rows, blocks, steps, own, pieces, ident, norm=None, before=None, before_steps=()):
    count, width = rows.shape
    wide = sum(b.shape[1] for b in blocks)
    final = norm is not None
    extra = []
    if final:
        residual, gain, bias = norm
        extra += [residual, gain.reshape(1, -1), bias.reshape(1, -1)]
    if before is not None:
        extra.append(before)
    depth = residual.shape[1] if final else wide
    return pl.pallas_call(
        functools.partial(scatter_kernel, tuple(steps), tuple(before_steps), final, pieces),
        in_specs=[pl.BlockSpec(memory_space=pltpu.VMEM)] * (1 + len(extra) + len(blocks)),
        out_specs=pl.BlockSpec(memory_space=pltpu.VMEM),
        out_shape=jax.ShapeDtypeStruct((own, depth), jnp.bfloat16 if final else jnp.float32),
        scratch_shapes=[
            pltpu.VMEM((4, own, wide), jnp.bfloat16),
            pltpu.VMEM((2, own, wide), jnp.bfloat16),
            pltpu.VMEM((own, wide), jnp.bfloat16),
            pltpu.VMEM((own, wide), jnp.bfloat16),
            pltpu.VMEM((own, depth) if final else (8, 128), jnp.float32),
            pltpu.SemaphoreType.DMA((3, pieces)),
            pltpu.SemaphoreType.DMA((3, pieces)),
        ],
        compiler_params=pltpu.CompilerParams(
            collective_id=ident, has_side_effects=True, vmem_limit_bytes=48 * 2**20
        ),
        cost_estimate=pl.CostEstimate(
            flops=25 * 10**9, bytes_accessed=16 * 2**20, transcendentals=0
        ),
        name=f"scatter_{ident}",
    )(rows, *extra, *blocks)


def gather_kernel(pieces, first_ref, out_ref, local, send, recv):
    me, partner, across, _ = places()
    block_rows = first_ref.shape[0]
    size = block_rows // pieces
    greet(partner, across)

    def copy(kind, s):
        owner = across if kind == 2 else me
        cut = pl.ds(pl.multiple_of(owner * block_rows + s * size, size), size)
        src = out_ref.at[cut] if kind == 2 else first_ref.at[pl.ds(s * size, size)]
        target = across if kind == 0 else partner
        return remote(src, out_ref.at[cut], send.at[kind, s], recv.at[kind, s], target)

    for s in range(pieces):
        copy(0, s).start()
    for s in range(pieces):
        copy(1, s).start()
    keep = pltpu.make_async_copy(
        first_ref,
        out_ref.at[pl.ds(pl.multiple_of(me * block_rows, block_rows), block_rows)],
        local,
    )
    keep.start()
    for s in range(pieces):
        copy(0, s).wait_recv()
        copy(2, s).start()
    for s in range(pieces):
        copy(1, s).wait_recv()
        copy(2, s).wait_recv()
    for s in range(pieces):
        for kind in range(3):
            copy(kind, s).wait_send()
    keep.wait()


def gather_rows(first, groups, pieces, ident):
    own, depth = first.shape
    return pl.pallas_call(
        functools.partial(gather_kernel, pieces),
        in_specs=[pl.BlockSpec(memory_space=pltpu.VMEM)],
        out_specs=pl.BlockSpec(memory_space=pltpu.VMEM),
        out_shape=jax.ShapeDtypeStruct((own * groups, depth), jnp.bfloat16),
        scratch_shapes=[
            pltpu.SemaphoreType.DMA,
            pltpu.SemaphoreType.DMA((3, pieces)),
            pltpu.SemaphoreType.DMA((3, pieces)),
        ],
        compiler_params=pltpu.CompilerParams(
            collective_id=ident, has_side_effects=True, vmem_limit_bytes=24 * 2**20
        ),
        cost_estimate=pl.CostEstimate(
            flops=25 * 10**9, bytes_accessed=5 * 2**20, transcendentals=0
        ),
        name="gather_rows",
    )(first)


def on_device(
    residual_in,
    queries,
    keys_values,
    sink_logit,
    out_weight,
    norm1_gain,
    norm1_bias,
    up_weight,
    down_weight,
    norm2_gain,
    norm2_bias,
):
    devices = lax.axis_size("sp")
    order = ring_order(devices)
    right = [(order[i], order[(i + 1) % devices]) for i in range(devices)]
    left = [(j, i) for i, j in right]
    far = devices // 2

    def hop(h, back, ahead):
        if h > far:
            return None, None
        if 2 * h == devices:
            half = back.shape[0] // 2
            return (
                lax.ppermute(back[:half], "sp", right),
                lax.ppermute(ahead[half:], "sp", left),
            )
        return lax.ppermute(back, "sp", right), lax.ppermute(ahead, "sp", left)

    tok_rows = queries.shape[0]
    me = lax.axis_index("sp")
    offset = me * tok_rows
    total = tok_rows * devices

    place = [0] * devices
    for p, d in enumerate(order):
        place[d] = p
    steps = [0]
    for h in range(1, far + 1):
        steps.append(-h)
        if 2 * h != devices:
            steps.append(h)
    table = jnp.array(
        [[order[(place[d] + s) % devices] for s in steps] for d in range(devices)], jnp.int32
    )
    owners = lax.dynamic_index_in_dim(table, me, 0, keepdims=False)
    starts = owners * up_weight.shape[0]

    if up_weight.shape[0] % 128:
        up_weight = lax.all_gather(up_weight, "sp", axis=0, tiled=True)
        down_weight = lax.all_gather(down_weight, "sp", axis=1, tiled=True)
        far, starts = 0, jnp.zeros((1,), jnp.int32)

    ups, downs = [up_weight], [down_weight]
    state = {"up": (up_weight, up_weight), "down": (down_weight, down_weight)}

    def advance(name, h):
        state[name] = hop(h, *state[name])

    def settle(name, h, *others):
        got = state[name]
        if got[0] is None or h > far:
            return others
        out = lax.optimization_barrier((*got, *others))
        state[name] = out[:2]
        blocks = ups if name == "up" else downs
        if 2 * h == devices:
            blocks.append(jnp.concatenate(out[:2], axis=0))
        else:
            blocks.extend(out[:2])
        return out[2:]

    own = residual_in.shape[0]
    advance("up", 1)
    padded = halo(keys_values, "sp", WINDOW)
    attended = attend(queries, padded, sink_logit, offset, total)
    (attended, down_own) = settle("up", 1, attended, down_weight)
    advance("up", 2)
    state["down"] = (down_own, down_own)
    advance("down", 1)
    first = scatter(
        attended, [out_weight], [0], own, 2, 0, (residual_in, norm1_gain, norm1_bias)
    )
    (first,) = settle("up", 2, first)
    advance("up", 3)
    rows = gather_rows(first, lax.axis_size("tp"), 4, 1)
    (rows,) = settle("down", 1, rows)
    (rows, *ready) = settle("up", 3, rows, *state["down"])
    state["down"] = tuple(ready)
    advance("up", 4)
    advance("down", 2)
    (rows,) = settle("up", 4, rows)
    for h in range(5, far + 1):
        advance("up", h)
        (rows,) = settle("up", h, rows)
    activation = up_project(rows, ups, starts)
    (activation,) = settle("down", 2, activation)
    advance("down", 3)
    early, tail = 0, None
    if far > 2:
        early = len(downs)
        tail = scatter(activation, downs, steps[:early], own, 2, 2)
        (tail,) = settle("down", 3, tail)
    for h in range(4, far + 1):
        advance("down", h)
        (activation, tail) = settle("down", h, activation, tail)
    return scatter(
        activation,
        downs[early:],
        steps[early : len(downs)],
        own,
        2,
        3,
        (first, norm2_gain, norm2_bias),
        tail,
        steps[:early],
    )


def solution(mesh):
    return jax.shard_map(
        on_device,
        mesh=mesh,
        in_specs=(
            P(("sp", "tp"), None),
            P("sp", "tp"),
            P(None, "sp", "tp"),
            P("tp"),
            P("tp", None),
            P(),
            P(),
            P("sp", "tp"),
            P("tp", "sp"),
            P(),
            P(),
        ),
        out_specs=P(("sp", "tp"), None),
        check_vma=False,
    )
```

```python
import functools

import jax
import jax.numpy as jnp
from jax import lax
from jax.experimental import pallas as pl
from jax.experimental.pallas import tpu as pltpu
from jax.sharding import PartitionSpec as P


HEAD_DIM = 64
WINDOW = 128
BLOCK = 256


def ring_order(devices):
    return list(range(0, devices, 2)) + list(range(1, devices, 2))[::-1]


def halo(shard, axis, width):
    devices, length = lax.axis_size(axis), shard.shape[1]
    up = [(i, (i + 1) % devices) for i in range(devices - 1)]
    down = [(j, i) for i, j in up]
    before = lax.ppermute(shard[:, length - width :], axis, up)
    after = lax.ppermute(shard[:, :width], axis, down)
    return jnp.concatenate([before, shard, after], axis=1)


def norm_rows(values, gain, bias):
    mean = jnp.mean(values, axis=-1, keepdims=True)
    centred = values - mean
    variance = jnp.mean(centred * centred, axis=-1, keepdims=True)
    return (centred * lax.rsqrt(variance + 1e-06) * gain + bias).astype(jnp.bfloat16)


def attend_kernel(total, heads, group, info_ref, sink_ref, q_ref, kv_ref, o_ref):
    start = pl.program_id(0) * BLOCK
    span = BLOCK + 2 * WINDOW
    rows = lax.broadcasted_iota(jnp.int32, (BLOCK, span), 0)
    cols = lax.broadcasted_iota(jnp.int32, (BLOCK, span), 1)
    pos = cols + (info_ref[0] + start - WINDOW)
    valid = (cols >= rows) & (cols - rows <= 2 * WINDOW) & (pos >= 0) & (pos < total)
    begin = pl.multiple_of(start, BLOCK)
    for kv in range(heads // group):
        lanes = slice(kv * HEAD_DIM, (kv + 1) * HEAD_DIM)
        keys = kv_ref[0, pl.ds(begin, span), lanes]
        values = kv_ref[1, pl.ds(begin, span), lanes]
        for sub in range(group):
            head = kv * group + sub
            mine = slice(head * HEAD_DIM, (head + 1) * HEAD_DIM)
            query = q_ref[:, mine]
            scores = lax.dot_general(
                query, keys, (((1,), (1,)), ((), ())), preferred_element_type=jnp.float32
            ) * HEAD_DIM ** (-0.5)
            scores = jnp.where(valid, scores, -jnp.inf)
            sink = sink_ref[head]
            top = jnp.maximum(jnp.max(scores, axis=-1, keepdims=True), sink)
            expd = jnp.exp(scores - top)
            denom = jnp.sum(expd, axis=-1, keepdims=True) + jnp.exp(sink - top)
            weights = (expd * (1.0 / denom)).astype(jnp.bfloat16)
            mixed = jnp.dot(weights, values, preferred_element_type=jnp.float32)
            o_ref[:, mine] = mixed.astype(jnp.bfloat16)


def attend(queries, padded, sink_logit, offset, total):
    rows, width = queries.shape
    heads = width // HEAD_DIM
    group = heads // (padded.shape[2] // HEAD_DIM)
    span = BLOCK + 2 * WINDOW
    flops = 4 * rows * span * width
    return pl.pallas_call(
        functools.partial(attend_kernel, total, heads, group),
        grid=(rows // BLOCK,),
        in_specs=[
            pl.BlockSpec(memory_space=pltpu.SMEM),
            pl.BlockSpec(memory_space=pltpu.SMEM),
            pl.BlockSpec((BLOCK, width), lambda i: (i, 0)),
            pl.BlockSpec(padded.shape, lambda i: (0, 0, 0)),
        ],
        out_specs=pl.BlockSpec((BLOCK, width), lambda i: (i, 0)),
        out_shape=jax.ShapeDtypeStruct((rows, width), jnp.bfloat16),
        compiler_params=pltpu.CompilerParams(vmem_limit_bytes=40 * 2**20),
        cost_estimate=pl.CostEstimate(
            flops=flops * 20, bytes_accessed=12 * 2**20, transcendentals=rows * span * heads
        ),
        name="attend",
    )(offset.reshape(1), sink_logit, queries, padded)


def up_kernel(info_ref, rows_ref, *refs):
    *blocks, out_ref = refs
    tile = 256
    for at in range(0, rows_ref.shape[0], tile):
        total = None
        for k, block in enumerate(blocks):
            depth = block.shape[0]
            begin = pl.multiple_of(info_ref[k], depth)
            term = jnp.dot(
                rows_ref[at : at + tile, pl.ds(begin, depth)],
                block[...],
                preferred_element_type=jnp.float32,
            )
            total = term if total is None else total + term
        out_ref[at : at + tile, :] = jnp.square(jnp.maximum(total, 0.0)).astype(jnp.bfloat16)


def up_project(rows, blocks, starts):
    count, depth = rows.shape
    hidden = blocks[0].shape[1]
    tile = min(512, hidden)
    return pl.pallas_call(
        up_kernel,
        grid=(hidden // tile,),
        in_specs=[
            pl.BlockSpec(memory_space=pltpu.SMEM),
            pl.BlockSpec(rows.shape, lambda j: (0, 0)),
        ]
        + [pl.BlockSpec((b.shape[0], tile), lambda j: (0, j)) for b in blocks],
        out_specs=pl.BlockSpec((count, tile), lambda j: (0, j)),
        out_shape=jax.ShapeDtypeStruct((count, hidden), jnp.bfloat16),
        compiler_params=pltpu.CompilerParams(vmem_limit_bytes=40 * 2**20),
        cost_estimate=pl.CostEstimate(
            flops=2 * count * depth * hidden, bytes_accessed=16 * 2**20, transcendentals=0
        ),
        name="up_project",
    )(starts, rows, *blocks)


MESH = pl.DeviceIdType.MESH


def remote(src, dst, send, recv, target):
    return pltpu.make_async_remote_copy(
        src_ref=src,
        dst_ref=dst,
        send_sem=send,
        recv_sem=recv,
        device_id={"tp": target},
        device_id_type=MESH,
    )


def places():
    me = lax.axis_index("tp")
    side, core = me // 2, me % 2
    return me, 2 * side + (1 - core), 2 * (1 - side) + core, 2 * (1 - side) + (1 - core)


def greet(*others):
    barrier = pltpu.get_barrier_semaphore()
    for other in others:
        pl.semaphore_signal(barrier, inc=1, device_id={"tp": other}, device_id_type=MESH)
    pl.semaphore_wait(barrier, len(others))


def ring_place(index, devices):
    odd = index % 2
    return (1 - odd) * (index // 2) + odd * (devices - 1 - index // 2)


def ring_device(place, devices):
    half = (devices + 1) // 2
    back = place // half
    return (1 - back) * (2 * place) + back * (2 * (devices - 1 - place) + 1)


def scatter_kernel(steps, before, final, pieces, rows_ref, *refs):
    refs = list(refs)
    if final:
        res_ref, gain_ref, bias_ref = refs[:3]
        refs = refs[3:]
    if before:
        before_ref = refs.pop(0)
    *blocks, out_ref, part, inc, total, got, whole, send, recv = refs
    me, partner, across, diagonal = places()
    block_rows = out_ref.shape[0]
    size = block_rows // pieces
    wide = blocks[0].shape[1]
    devices = lax.axis_size("sp")
    spot = ring_place(lax.axis_index("sp"), devices)
    greet(partner, across)

    def compute(slot, owner, s):
        begin = pl.multiple_of(owner * block_rows + s * size, size)
        mine = rows_ref[pl.ds(begin, size), :]
        for k, block in enumerate(blocks):
            part[slot, pl.ds(s * size, size), k * wide : (k + 1) * wide] = jnp.dot(
                mine, block[...], preferred_element_type=jnp.float32
            ).astype(jnp.bfloat16)

    def copy(kind, s):
        cut = pl.ds(s * size, size)
        if kind == 0:
            src, dst, target = part.at[0, cut], inc.at[0, cut], partner
        elif kind == 1:
            src, dst, target = total.at[cut], got.at[cut], across
        else:
            src, dst, target = part.at[2, cut], inc.at[1, cut], partner
        return remote(src, dst, send.at[kind, s], recv.at[kind, s], target)

    def column(step):
        if wide == whole.shape[1]:
            return pl.ds(0, wide)
        at = ring_device((spot + step + devices) % devices, devices) * wide
        return pl.ds(pl.multiple_of(at, wide), wide)

    for s in range(pieces):
        cut = pl.ds(s * size, size)
        compute(0, diagonal, s)
        copy(0, s).start()
        compute(1, across, s)
        copy(0, s).wait_recv()
        total[cut, :] = (
            part[1, cut, :].astype(jnp.float32) + inc[0, cut, :].astype(jnp.float32)
        ).astype(jnp.bfloat16)
        copy(1, s).start()
    for s in range(pieces):
        compute(2, partner, s)
        copy(2, s).start()
    for s in range(pieces):
        compute(3, me, s)
    for s in range(pieces):
        copy(2, s).wait_recv()
        if final:
            for k, step in enumerate(before):
                at = column(step)
                cut = pl.ds(s * size, size)
                whole[cut, at] = (
                    res_ref[cut, at].astype(jnp.float32)
                    + before_ref[cut, k * wide : (k + 1) * wide]
                )
    for s in range(pieces):
        cut = pl.ds(s * size, size)
        copy(1, s).wait_recv()
        for k, step in enumerate(steps):
            mine = slice(k * wide, (k + 1) * wide)
            here = (
                part[3, cut, mine].astype(jnp.float32)
                + inc[1, cut, mine].astype(jnp.float32)
                + got[cut, mine].astype(jnp.float32)
            )
            if final:
                at = column(step)
                whole[cut, at] = res_ref[cut, at].astype(jnp.float32) + here
            else:
                out_ref[cut, mine] = here
        if final:
            out_ref[cut, :] = norm_rows(whole[cut, :], gain_ref[...], bias_ref[...])
    for s in range(pieces):
        for kind in range(3):
            copy(kind, s).wait_send()


def scatter(rows, blocks, steps, own, pieces, ident, norm=None, before=None, before_steps=()):
    wide = sum(b.shape[1] for b in blocks)
    final = norm is not None
    extra = []
    if final:
        residual, gain, bias = norm
        extra += [residual, gain.reshape(1, -1), bias.reshape(1, -1)]
    if before is not None:
        extra.append(before)
    depth = residual.shape[1] if final else wide
    return pl.pallas_call(
        functools.partial(scatter_kernel, tuple(steps), tuple(before_steps), final, pieces),
        in_specs=[pl.BlockSpec(memory_space=pltpu.VMEM)] * (1 + len(extra) + len(blocks)),
        out_specs=pl.BlockSpec(memory_space=pltpu.VMEM),
        out_shape=jax.ShapeDtypeStruct((own, depth), jnp.bfloat16 if final else jnp.float32),
        scratch_shapes=[
            pltpu.VMEM((4, own, wide), jnp.bfloat16),
            pltpu.VMEM((2, own, wide), jnp.bfloat16),
            pltpu.VMEM((own, wide), jnp.bfloat16),
            pltpu.VMEM((own, wide), jnp.bfloat16),
            pltpu.VMEM((own, depth) if final else (8, 128), jnp.float32),
            pltpu.SemaphoreType.DMA((3, pieces)),
            pltpu.SemaphoreType.DMA((3, pieces)),
        ],
        compiler_params=pltpu.CompilerParams(
            collective_id=ident, has_side_effects=True, vmem_limit_bytes=48 * 2**20
        ),
        cost_estimate=pl.CostEstimate(
            flops=25 * 10**9, bytes_accessed=16 * 2**20, transcendentals=0
        ),
    )(rows, *extra, *blocks)


def gather_kernel(pieces, first_ref, out_ref, local, send, recv):
    me, partner, across, _ = places()
    block_rows = first_ref.shape[0]
    size = block_rows // pieces
    greet(partner, across)

    def copy(kind, s):
        owner = across if kind == 2 else me
        cut = pl.ds(pl.multiple_of(owner * block_rows + s * size, size), size)
        src = out_ref.at[cut] if kind == 2 else first_ref.at[pl.ds(s * size, size)]
        target = across if kind == 0 else partner
        return remote(src, out_ref.at[cut], send.at[kind, s], recv.at[kind, s], target)

    for s in range(pieces):
        copy(0, s).start()
    for s in range(pieces):
        copy(1, s).start()
    keep = pltpu.make_async_copy(
        first_ref,
        out_ref.at[pl.ds(pl.multiple_of(me * block_rows, block_rows), block_rows)],
        local,
    )
    keep.start()
    for s in range(pieces):
        copy(0, s).wait_recv()
        copy(2, s).start()
    for s in range(pieces):
        copy(1, s).wait_recv()
        copy(2, s).wait_recv()
    for s in range(pieces):
        for kind in range(3):
            copy(kind, s).wait_send()
    keep.wait()


def gather_rows(first, groups, pieces, ident):
    own, depth = first.shape
    return pl.pallas_call(
        functools.partial(gather_kernel, pieces),
        in_specs=[pl.BlockSpec(memory_space=pltpu.VMEM)],
        out_specs=pl.BlockSpec(memory_space=pltpu.VMEM),
        out_shape=jax.ShapeDtypeStruct((own * groups, depth), jnp.bfloat16),
        scratch_shapes=[
            pltpu.SemaphoreType.DMA,
            pltpu.SemaphoreType.DMA((3, pieces)),
            pltpu.SemaphoreType.DMA((3, pieces)),
        ],
        compiler_params=pltpu.CompilerParams(
            collective_id=ident, has_side_effects=True, vmem_limit_bytes=24 * 2**20
        ),
        cost_estimate=pl.CostEstimate(
            flops=25 * 10**9, bytes_accessed=5 * 2**20, transcendentals=0
        ),
        name="gather_rows",
    )(first)


def on_device(
    residual_in,
    queries,
    keys_values,
    sink_logit,
    out_weight,
    norm1_gain,
    norm1_bias,
    up_weight,
    down_weight,
    norm2_gain,
    norm2_bias,
):
    devices = lax.axis_size("sp")
    order = ring_order(devices)
    right = [(order[i], order[(i + 1) % devices]) for i in range(devices)]
    left = [(j, i) for i, j in right]
    far = devices // 2

    def hop(h, back, ahead):
        if h > far:
            return None, None
        if 2 * h == devices:
            half = back.shape[0] // 2
            back, ahead = back[:half], ahead[half:]
        back = lax.ppermute(back, "sp", right)
        ahead = lax.ppermute(ahead, "sp", left)
        return back, ahead

    tok_rows = queries.shape[0]
    me = lax.axis_index("sp")
    offset = me * tok_rows
    total = tok_rows * devices

    place = [0] * devices
    for p, d in enumerate(order):
        place[d] = p
    steps = [0]
    for h in range(1, far + 1):
        steps.append(-h)
        if 2 * h != devices:
            steps.append(h)
    table = jnp.array(
        [[order[(place[d] + s) % devices] for s in steps] for d in range(devices)], jnp.int32
    )
    owners = lax.dynamic_index_in_dim(table, me, 0, keepdims=False)
    starts = owners * up_weight.shape[0]

    if up_weight.shape[0] % 128:
        up_weight = lax.all_gather(up_weight, "sp", axis=0, tiled=True)
        down_weight = lax.all_gather(down_weight, "sp", axis=1, tiled=True)
        far, starts = 0, jnp.zeros((1,), jnp.int32)

    ups, downs = [up_weight], [down_weight]
    state = {"up": (up_weight, up_weight), "down": (down_weight, down_weight)}

    def advance(name, h):
        state[name] = hop(h, *state[name])

    def settle(name, h, *others):
        got = state[name]
        if got[0] is None or h > far:
            return others
        out = lax.optimization_barrier((*got, *others))
        state[name] = out[:2]
        blocks = ups if name == "up" else downs
        if 2 * h == devices:
            blocks.append(jnp.concatenate(out[:2], axis=0))
        else:
            blocks.extend(out[:2])
        return out[2:]

    own = residual_in.shape[0]
    advance("up", 1)
    padded = halo(keys_values, "sp", WINDOW)
    attended = attend(queries, padded, sink_logit, offset, total)
    (attended, down_own) = settle("up", 1, attended, down_weight)
    advance("up", 2)
    state["down"] = (down_own, down_own)
    advance("down", 1)
    first = scatter(
        attended, [out_weight], [0], own, 2, 0, (residual_in, norm1_gain, norm1_bias)
    )
    (first,) = settle("up", 2, first)
    advance("up", 3)
    rows = gather_rows(first, lax.axis_size("tp"), 4, 1)
    (rows,) = settle("down", 1, rows)
    (rows, *ready) = settle("up", 3, rows, *state["down"])
    state["down"] = tuple(ready)
    advance("up", 4)
    advance("down", 2)
    (rows,) = settle("up", 4, rows)
    for h in range(5, far + 1):
        advance("up", h)
        (rows,) = settle("up", h, rows)
    activation = up_project(rows, ups, starts)
    (activation,) = settle("down", 2, activation)
    advance("down", 3)
    early, tail = 0, None
    if far > 2:
        early = len(downs)
        tail = scatter(activation, downs, steps[:early], own, 2, 2)
        (tail,) = settle("down", 3, tail)
    for h in range(4, far + 1):
        advance("down", h)
        (activation, tail) = settle("down", h, activation, tail)
    return scatter(
        activation,
        downs[early:],
        steps[early : len(downs)],
        own,
        2,
        3,
        (first, norm2_gain, norm2_bias),
        tail,
        steps[:early],
    )


def solution(mesh):
    return jax.shard_map(
        on_device,
        mesh=mesh,
        in_specs=(
            P(("sp", "tp"), None),
            P("sp", "tp"),
            P(None, "sp", "tp"),
            P("tp"),
            P("tp", None),
            P(),
            P(),
            P("sp", "tp"),
            P("tp", "sp"),
            P(),
            P(),
        ),
        out_specs=P(("sp", "tp"), None),
        check_vma=False,
    )
```
